512 devices in a mesh: kv: 16 (over y, x), tp: 32 (over z, core).
Axes of the slice: x: 4, y: 4, z: 16, core: 2. Of those that a mesh axis runs over, the one named last changes fastest.
Arguments:
- hidden_in: bfloat16 [64, 4096], P('kv', 'tp'), may hold values from -12 to 12
- mixer_gain: float32 [4096], P('tp'), may hold values from 0.1 to 1.9
- query_weight: bfloat16 [4096, 4096], P('tp', 'kv'), may hold values from -0.09375 to 0.09375
- key_weight: bfloat16 [4096, 4096], P('tp', 'kv'), may hold values from -0.09375 to 0.09375
- value_weight: bfloat16 [4096, 8192], P('tp', 'kv'), may hold values from -0.09375 to 0.09375
- gate_weight: bfloat16 [4096, 8192], P('tp', 'kv'), may hold values from -0.09375 to 0.09375
- decay_rate: float32 [16], P('kv'), may hold values from 0.0005 to 0.15
- prior_state: float32 [64, 16, 256, 512], P('tp', 'kv'), may hold values from -2.5 to 2.5
- key_block: bfloat16 [64, 16, 128, 256], P('tp', 'kv'), may hold values from -1 to 1
- value_block: bfloat16 [64, 16, 128, 512], P('tp', 'kv'), may hold values from -6 to 6
- lengths: int32 [64], P('tp'), may hold values from 1 to 16384, 262144 in all
- group_gain: float32 [8192], P('kv'), may hold values from 0.1 to 1.9
- output_weight: bfloat16 [8192, 4096], P('kv', 'tp'), may hold values from -0.0625 to 0.0625
- channel_gain: float32 [4096], P('tp'), may hold values from 0.1 to 1.9
- hidden_gate: bfloat16 [4096, 11264], P('tp', 'kv'), may hold values from -0.09375 to 0.09375
- hidden_up: bfloat16 [4096, 11264], P('tp', 'kv'), may hold values from -0.09375 to 0.09375
- hidden_down: bfloat16 [11264, 4096], P('kv', 'tp'), may hold values from -0.0546875 to 0.0546875
Outputs:
- layer_out: bfloat16 [64, 4096], P('kv', 'tp')
The draws below stay inside these ranges and needn't reach their ends.
Inputs may be any that keep to these rules, and one draw needn't show every extreme that they name: Sequence s has lengths[s] earlier positions; slots 0 to (lengths[s] mod 128) - 1 of key_block and value_block hold the turned, scaled keys and the values of its positions from 128 * floor(lengths[s] / 128) on, prior_state holds the state of the positions before them, and the other slots take no part.
All inputs are finite; a program needn't handle non-finite values. No bound on the sum of `lengths` on one device may be relied on, other than what follows from the above.
Results may differ from the reference program's by a relative error of at most 0.029.
Values may be sent and summed in bfloat16 or wider, within the bound.
A program may use at most 64 MiB of HBM per device.

```python
import math
import jax
import jax.numpy as jnp
import numpy as np
from jax import lax

D = 4096
HEADS = 16
DK = 256
DV = 512
FF = 11264
BLK = 128
MEAN_LEN = 4096
MOST_LEN = 16384
SEQS = 64


def draw_hidden_in(key, part):
    columns = jnp.arange(D, dtype=jnp.float32) / D
    column_scale = 0.4 * jnp.exp(jnp.log(5.0) * columns)
    base_key = jax.random.fold_in(key, 11)
    base = jnp.clip(jax.random.normal(base_key, (SEQS, D), jnp.float32), -6.0, 6.0)
    return (base * column_scale[None, :]).astype(jnp.bfloat16)


def draw_decay_rate(key, part):
    lowest_rate = 0.003
    highest_rate = 0.15
    uniform_unit = jax.random.uniform(jax.random.fold_in(key, 21), (HEADS,), jnp.float32)
    return jnp.exp(jnp.log(lowest_rate) + uniform_unit * (jnp.log(highest_rate) - jnp.log(lowest_rate)))


def steps_of(own_key, extent, pieces, smallest, high):
    gain = 1.0
    for dim, shards_of in pieces:
        draws = jax.random.uniform(jax.random.fold_in(jax.random.fold_in(own_key, 6), dim), (shards_of,), jnp.float32, smallest / len(pieces), high / len(pieces))
        gain = gain * jnp.repeat(jnp.exp(draws), extent[dim] // shards_of).reshape((-1,) + (1,) * (len(extent) - 1 - dim))
    return gain


def length_profile(number_of, total, limit, lean):
    weights = [(1 << 20) // math.isqrt(standing ** lean) + 1 for standing in range(2, number_of + 1)]
    spare, counts = total - limit - (number_of - 1), [1] * (number_of - 1)
    while spare > 0:
        free = [i for i in range(number_of - 1) if counts[i] < limit]
        whole, budget = sum([weights[i] for i in free]), spare
        for i in free:
            extra = min(limit - counts[i], max(1, budget * weights[i] // whole), spare)
            counts[i] = counts[i] + extra
            spare = spare - extra
    return np.array([limit] + counts)


def uneven_parts(key, number_of, total, limit, skew):
    if number_of == 2:
        one = jax.random.randint(key, (), max(1, total - limit), min(limit, total - 1) + 1)
        return jnp.stack([one, total - one])
    sizes = jnp.asarray(length_profile(number_of, total, limit, skew), jnp.int32)
    couples = (number_of - 1) // 2
    giver, taker = sizes[1:1 + 2 * couples:2], sizes[2:2 + 2 * couples:2]
    room = jnp.minimum(giver - 1, limit - taker)
    shifted = jax.random.randint(jax.random.fold_in(key, 1), (couples,), 0, 1 << 20) % (room + 1)
    sizes = sizes.at[1:1 + 2 * couples:2].set(giver - shifted).at[2:2 + 2 * couples:2].set(taker + shifted)
    return sizes[jax.random.permutation(jax.random.fold_in(key, 2), number_of)]


def bell_draw(stream_key, extent, deviation, limit, split=(), kind=jnp.bfloat16):
    drawn = jax.random.normal(stream_key, extent, jnp.float32) * deviation
    if len(split) > 0:
        drawn = steps_of(stream_key, extent, split, -0.22, 0.18) * drawn
    return jnp.clip(drawn, min=-limit, max=limit).astype(kind)


def setup_inputs(seed: int = 0) -> dict:
    keys = jax.random.split(jax.random.key(seed), 18)
    return {
        "hidden_in": draw_hidden_in(jax.random.fold_in(keys[17], 71), 0),
        "mixer_gain": jnp.clip(1.0 + 0.18 * jax.random.normal(keys[1], (D,), jnp.float32), 0.1, 1.9),
        "query_weight": bell_draw(keys[2], (D, HEADS * DK), D ** -0.5, 0.09375, ((0, 32), (1, 16))),
        "key_weight": bell_draw(keys[3], (D, HEADS * DK), D ** -0.5, 0.09375, ((0, 32), (1, 16))),
        "value_weight": bell_draw(keys[4], (D, HEADS * DV), D ** -0.5, 0.09375, ((0, 32), (1, 16))),
        "gate_weight": bell_draw(keys[5], (D, HEADS * DV), D ** -0.5, 0.09375, ((0, 32), (1, 16))),
        "decay_rate": draw_decay_rate(jax.random.fold_in(keys[17], 71), 0),
        "prior_state": bell_draw(keys[7], (SEQS, HEADS, DK, DV), 0.3, 2.5, ((0, 32), (1, 16)), jnp.float32),
        "key_block": bell_draw(keys[8], (SEQS, HEADS, BLK, DK), 0.0625, 1.0, ((0, 32), (1, 16))),
        "value_block": bell_draw(keys[9], (SEQS, HEADS, BLK, DV), 1.0, 6.0, ((0, 32), (1, 16))),
        "lengths": uneven_parts(keys[10], SEQS, SEQS * MEAN_LEN, MOST_LEN, 2).astype(jnp.int32),
        "group_gain": jnp.clip(1.0 + 0.18 * jax.random.normal(keys[11], (HEADS * DV,), jnp.float32), 0.1, 1.9),
        "output_weight": bell_draw(keys[12], (HEADS * DV, D), (HEADS * DV) ** -0.5, 0.0625, ((0, 16), (1, 32))),
        "channel_gain": jnp.clip(1.0 + 0.18 * jax.random.normal(keys[13], (D,), jnp.float32), 0.1, 1.9),
        "hidden_gate": bell_draw(keys[14], (D, FF), D ** -0.5, 0.09375, ((0, 32), (1, 16))),
        "hidden_up": bell_draw(keys[15], (D, FF), D ** -0.5, 0.09375, ((0, 32), (1, 16))),
        "hidden_down": bell_draw(keys[16], (FF, D), FF ** -0.5, 0.0546875, ((0, 16), (1, 32))),
    }


epsilon = 1e-06

def rotate(vectors, position):
    half_dim = vectors.shape[-1] // 2
    inverse = 10000.0 ** (-jnp.arange(half_dim, dtype=jnp.float32) / half_dim)
    angles = position.astype(jnp.float32)[:, None, None] * inverse
    cosine_part = jnp.cos(angles)
    sine_part = jnp.sin(angles)
    front_half = vectors[..., :half_dim]
    back_half = vectors[..., half_dim:]
    return jnp.concatenate([front_half * cosine_part - back_half * sine_part, front_half * sine_part + back_half * cosine_part], axis=-1)

def retain(queries, keys_new, values_new, gates, decay_rate, prior_state, key_block, value_block, lengths, group_gain):
    batch_rows = queries.shape[0]
    heads_here = decay_rate.shape[0]
    key_width = prior_state.shape[2]
    value_width = prior_state.shape[3]
    block_len = key_block.shape[2]
    rotated = rotate(queries.astype(jnp.float32).reshape(batch_rows, heads_here, key_width), lengths).astype(jnp.bfloat16)
    fresh_keys = rotate(keys_new.astype(jnp.float32).reshape(batch_rows, heads_here, key_width), lengths) * key_width ** (-0.5)
    fresh_values = values_new.astype(jnp.float32).reshape(batch_rows, heads_here, value_width)
    filled = (lengths % block_len).astype(jnp.int32)
    slots = jnp.arange(block_len, dtype=jnp.int32)
    distance = (filled[:, None] - slots[None, :]).astype(jnp.float32)
    live_slots = (slots[None, :] < filled[:, None])[:, None, :]
    weighting = jnp.where(live_slots, jnp.exp(-decay_rate[None, :, None] * distance[:, None, :]), jnp.float32(0.0))
    rotated_wide = rotated.astype(jnp.float32)
    scores = jnp.einsum('shk,shjk->shj', rotated_wide, key_block.astype(jnp.float32))
    block_weights = (scores * weighting).astype(jnp.bfloat16)
    block_term = jnp.einsum('shj,shjv->shv', block_weights.astype(jnp.float32), value_block.astype(jnp.float32))
    own_term = lax.optimization_barrier(jnp.sum(rotated_wide * fresh_keys, axis=-1, keepdims=True)) * fresh_values
    carried = jnp.exp(-decay_rate[None, :, None] * (filled[:, None, None] + 1).astype(jnp.float32))
    state_term = carried * jnp.einsum('shk,shkv->shv', rotated_wide, prior_state, precision=lax.Precision.HIGHEST)
    retained = own_term + block_term + state_term
    centre = lax.optimization_barrier(jnp.mean(retained, axis=-1, keepdims=True))
    spread = lax.optimization_barrier(jnp.mean(jnp.square(retained - centre), axis=-1, keepdims=True))
    normed = (retained - centre) * lax.rsqrt(spread + epsilon)
    gated = jax.nn.silu(gates.astype(jnp.float32)).reshape(batch_rows, heads_here, value_width) * normed * group_gain.reshape(heads_here, value_width)
    return gated.astype(jnp.bfloat16).reshape(batch_rows, heads_here * value_width)

def reference(hidden_in, mixer_gain, query_weight, key_weight, value_weight, gate_weight, decay_rate, prior_state, key_block, value_block, lengths, group_gain, output_weight, channel_gain, hidden_gate, hidden_up, hidden_down):
    stream = hidden_in.astype(jnp.float32)
    first_scale = lax.rsqrt(lax.optimization_barrier(jnp.mean(stream * stream, axis=1, keepdims=True)) + epsilon)
    scaled_in = (stream * mixer_gain).astype(jnp.bfloat16)
    queries = (first_scale * jnp.dot(scaled_in, query_weight, preferred_element_type=jnp.float32)).astype(jnp.bfloat16)
    keys_new = (first_scale * jnp.dot(scaled_in, key_weight, preferred_element_type=jnp.float32)).astype(jnp.bfloat16)
    values_new = (first_scale * jnp.dot(scaled_in, value_weight, preferred_element_type=jnp.float32)).astype(jnp.bfloat16)
    gates = (first_scale * jnp.dot(scaled_in, gate_weight, preferred_element_type=jnp.float32)).astype(jnp.bfloat16)
    mixed = retain(queries, keys_new, values_new, gates, decay_rate, prior_state, key_block, value_block, lengths, group_gain)
    middle = stream + jnp.dot(mixed, output_weight, preferred_element_type=jnp.float32)
    second_scale = lax.rsqrt(lax.optimization_barrier(jnp.mean(middle * middle, axis=1, keepdims=True)) + epsilon)
    scaled_mid = (middle * channel_gain).astype(jnp.bfloat16)
    gate_part = second_scale * jnp.dot(scaled_mid, hidden_gate, preferred_element_type=jnp.float32)
    up_part = second_scale * jnp.dot(scaled_mid, hidden_up, preferred_element_type=jnp.float32)
    activated = (jax.nn.silu(gate_part) * up_part).astype(jnp.bfloat16)
    return (middle + jnp.dot(activated, hidden_down, preferred_element_type=jnp.float32)).astype(jnp.bfloat16)
```

```python
import functools

import jax
import jax.numpy as jnp
import numpy as np
from jax import lax
from jax.experimental import pallas as pl
from jax.experimental.pallas import tpu as pltpu
from jax.sharding import PartitionSpec as P

D = 4096
EPS = 1e-06
KV = 16
ZS = 16
TP = 32
DK = 256
DV = 512
FU = 704
FP = 768
MSG = 1664
F32 = jnp.float32
BF16 = jnp.bfloat16
MESH = pl.DeviceIdType.MESH

PLANE = sorted(
    [(dy, dx) for dy in range(4) for dx in range(4) if (dy, dx) != (0, 0)],
    key=lambda o: -(min(o[0], 4 - o[0]) + min(o[1], 4 - o[1])),
)


def dot(a, b):
    return jnp.dot(a, b, preferred_element_type=F32)


def sin_cos(a):
    n = jnp.floor(a * np.float32(2.0 / np.pi) + 0.5)
    r = a - n * np.float32(1.5703125)
    r = r - n * np.float32(4.837512969970703125e-4)
    r = r - n * np.float32(7.549789954891882e-8)
    z = r * r
    s = r + r * z * (-1.6666654611e-1 + z * (8.3321608736e-3 - z * 1.9515295891e-4))
    c = 1.0 - 0.5 * z + z * z * (
        4.166664568298827e-2 + z * (-1.388731625493765e-3 + z * 2.443315711809948e-5)
    )
    m = n - 4.0 * jnp.floor(n * 0.25)
    odd = (m == 1.0) | (m == 3.0)
    sine = jnp.where(odd, c, s)
    cosine = jnp.where(odd, s, c)
    sine = jnp.where(m >= 2.0, -sine, sine)
    cosine = jnp.where((m == 1.0) | (m == 2.0), -cosine, cosine)
    return sine, cosine


def kernel(
    hid, mgain, wq, wk, wv, wg, decay, state, kblk, vblk, lens, ggain, wo, cgain, hg, hu, hd, freq,
    out,
    hid_v, mg_v, w1, state_v, kb_v, vb_v, gg_v, wo_v, cg_v, w2g, w2u, wd_v, fr_v, len_s, dec_s,
    sh, sl, sin_v, cos_v, wt_v, carry_v,
    xg, xs, lhs1, sib_s, sib_r, msg, rb, mx, mgat, lhs_f, psend, pr, mid3, lhs2, sib_s2, sib_r2,
    msg2, rb2, act, agat, lhs_d, hmsg, hr,
    lsem, ssa, rsa, sspair, rspair, ssb, rsb, ssc, rsc, ssd, rsd, ssf, rsf, ssg, rsg, ssh, rsh,
    far,
):
    k = lax.axis_index("kv")
    t = lax.axis_index("tp")
    z, c = t // 2, t % 2
    y, x = k // 4, k % 4

    def kv_peer(dy, dx):
        return ((y + dy) % 4) * 4 + (x + dx) % 4

    def z_peer(i):
        off = 8 - (i + 1) // 2
        sign = (i % 2) * 2 - 1
        return (z + sign * off + 16) % 16

    loads = [
        (hid, hid_v), (lens, len_s), (decay, dec_s), (freq, fr_v), (mgain, mg_v),
        (wq, w1.at[:, pl.ds(0, 256)]), (wk, w1.at[:, pl.ds(256, 256)]),
        (wv, w1.at[:, pl.ds(512, 512)]), (wg, w1.at[:, pl.ds(1024, 512)]),
        (state, state_v), (kblk, kb_v), (vblk, vb_v), (ggain, gg_v), (wo, wo_v), (cgain, cg_v),
        (hg, w2g), (hu, w2u), (hd, wd_v),
    ]
    copies = [pltpu.make_async_copy(a, b, lsem.at[i]) for i, (a, b) in enumerate(loads)]
    for cp in copies:
        cp.start()

    barrier = pltpu.get_barrier_semaphore()
    for dy, dx in PLANE:
        pl.semaphore_signal(
            barrier, inc=1, device_id={"kv": kv_peer(dy, dx), "tp": t}, device_id_type=MESH
        )

    @pl.loop(0, 16)
    def _(i):
        dz = i % 8 + 1 - (i % 8) // 4 * 9
        peer = ((z + dz + 16) % 16) * 2 + i // 8
        pl.semaphore_signal(barrier, inc=1, device_id={"kv": k, "tp": peer}, device_id_type=MESH)

    pl.semaphore_signal(
        barrier, inc=1, device_id={"kv": k, "tp": 2 * z + 1 - c}, device_id_type=MESH
    )

    for i in (1, 2, 3):
        copies[i].wait()
    row = lax.broadcasted_iota(jnp.int32, (2, 128), 0)
    slot = lax.broadcasted_iota(jnp.int32, (2, 128), 1)
    length = jnp.where(row == 0, len_s[0], len_s[1])
    sine, cosine = sin_cos(length.astype(F32) * fr_v[...])
    sin_v[...] = sine
    cos_v[...] = cosine
    filled = length & 127
    rate = dec_s[0]
    wt_v[...] = jnp.where(
        slot < filled, jnp.exp(-rate * (filled - slot).astype(F32)), jnp.zeros((2, 128), F32)
    )
    carry_v[...] = jnp.exp(-rate * (filled + 1).astype(F32))

    copies[0].wait()
    pl.semaphore_wait(barrier, 32)

    def to(src, dst, ss, rs, kv, tp):
        return pltpu.make_async_remote_copy(
            src_ref=src, dst_ref=dst, send_sem=ss, recv_sem=rs,
            device_id={"kv": kv, "tp": tp}, device_id_type=MESH,
        )

    for dy, dx in PLANE:
        p = kv_peer(dy, dx)
        to(hid_v, xg.at[k], ssa.at[p], rsa.at[k], p, t).start()
    for sg in (4, 12):
        pl.semaphore_signal(
            far, inc=1, device_id={"kv": k, "tp": ((z + sg) % 16) * 2 + c}, device_id_type=MESH
        )
    xg[k] = hid_v[...]

    copies[9].wait()
    for s in range(2):
        whole = state_v[s, 0]
        high = whole.astype(BF16)
        sh[s] = high
        sl[s] = (whole - high.astype(F32)).astype(BF16)
    for i in (4, 5, 6, 7, 8):
        copies[i].wait()

    def plane_wait(src, dst, ss, rs, recv):
        for dy, dx in PLANE:
            p = kv_peer(dy, dx)
            cp = to(src(p), dst(p), ss.at[p], rs.at[p], p, t)
            cp.wait_recv() if recv else cp.wait_send()

    plane_wait(lambda p: hid_v, lambda p: xg.at[p], ssa, rsa, True)
    for i in range(KV):
        rows = xg[i].astype(F32)
        xs[2 * i : 2 * i + 2, :] = rows[0:2]
        xs[32 + 2 * i : 34 + 2 * i, :] = rows[2:4]

    stream = xs[...]
    scaled = (stream * mg_v[...][None, :]).astype(BF16)
    lhs1[0] = scaled[0:32]
    lhs1[1] = scaled[32:64]

    def reduce_rows(product, send, recv, which, msgs, rbuf, ss, rs, first):
        send[...] = product(1 - c).astype(BF16)
        sib = 2 * z + 1 - c
        pair = to(send, recv, sspair.at[which], rspair.at[which], k, sib)
        pair.start()
        mine = product(c)
        pair.wait()
        both = mine + recv[...].astype(F32)
        for i in range(ZS):
            msgs[i] = both[2 * i : 2 * i + 2, :].astype(BF16)
        if first:
            pl.semaphore_wait(far, 2)

        @pl.loop(0, 15)
        def _(i):
            p = z_peer(i)
            to(msgs.at[p], rbuf.at[z], ss.at[p], rs.at[z], k, 2 * p + c).start()

        rbuf[z] = msgs[z]

        @pl.loop(0, 15)
        def _(i):
            p = z_peer(14 - i)
            to(msgs.at[p], rbuf.at[p], ss.at[p], rs.at[p], k, 2 * p + c).wait_recv()

        total = rbuf[0].astype(F32)
        for i in range(1, ZS):
            total = total + rbuf[i].astype(F32)
        scale = lax.rsqrt(
            jnp.sum(total[:, 1536:1664], axis=1, keepdims=True) * np.float32(1.0 / D) + EPS
        )
        return total, scale

    def sends_done(msgs, rbuf, ss, rs):
        @pl.loop(0, 15)
        def _(i):
            p = z_peer(i)
            to(msgs.at[p], rbuf.at[p], ss.at[p], rs.at[p], k, 2 * p + c).wait_send()

    def product1(i):
        left = lhs1[i]
        rows = xs[pl.ds(pl.multiple_of(i * 32, 32), 32), :]
        return jnp.concatenate([dot(left, w1[...]), rows * rows], axis=1)

    total, scale = reduce_rows(product1, sib_s, sib_r, 0, msg, rb, ssb, rsb, True)

    def rounded(v):
        return (scale * v).astype(BF16).astype(F32)

    queries, keys_new = rounded(total[:, 0:256]), rounded(total[:, 256:512])
    values_new, gates = rounded(total[:, 512:1024]), rounded(total[:, 1024:1536])
    sine, cosine = sin_v[...], cos_v[...]

    def rotate(v):
        a, b = v[:, 0:128], v[:, 128:256]
        return jnp.concatenate([a * cosine - b * sine, a * sine + b * cosine], axis=1)

    rot = rotate(queries).astype(BF16)
    rot_w = rot.astype(F32)
    fresh = rotate(keys_new) * np.float32(DK**-0.5)
    for i in (10, 11, 12):
        copies[i].wait()

    def pick(a, b):
        first = lax.broadcasted_iota(jnp.int32, a.shape, 0) == 0
        return jnp.where(first, a, b)

    scores = pick(*[
        lax.dot_general(rot, kb_v[s, 0], (((1,), (1,)), ((), ())), preferred_element_type=F32)
        for s in range(2)
    ])
    bw = (scores * wt_v[...]).astype(BF16)
    block_term = pick(*[dot(bw, vb_v[s, 0]) for s in range(2)])
    state_term = pick(*[dot(rot, sh[s]) + dot(rot, sl[s]) for s in range(2)])
    own_term = jnp.sum(rot_w * fresh, axis=1, keepdims=True) * values_new
    retained = own_term + block_term + carry_v[:, 0:1] * state_term
    centre = jnp.mean(retained, axis=1, keepdims=True)
    off = retained - centre
    spread = jnp.mean(off * off, axis=1, keepdims=True)
    normed = off * lax.rsqrt(spread + EPS)
    silu = gates / (1.0 + jnp.exp(-gates))
    mx[...] = (silu * normed * gg_v[...][None, :]).astype(BF16)

    def tp_gather(src, buf, ss, rs):
        @pl.loop(0, 15)
        def _(i):
            p = z_peer(i)
            for core in range(2):
                to(src, buf.at[t], ss.at[2 * p + core], rs.at[t], k, 2 * p + core).start()

        sib = 2 * z + 1 - c
        to(src, buf.at[t], ss.at[sib], rs.at[t], k, sib).start()
        buf[t] = src[...]

    def tp_wait(src, buf, ss, rs, recv):
        @pl.loop(1, 32)
        def _(i):
            p = (t + i) % 32
            cp = to(src, buf.at[p], ss.at[p], rs.at[p], k, p)
            cp.wait_recv() if recv else cp.wait_send()

    tp_gather(mx, mgat, ssc, rsc)
    plane_wait(lambda p: hid_v, lambda p: xg.at[p], ssa, rsa, False)
    sends_done(msg, rb, ssb, rsb)
    for i in (13, 14, 15, 16, 17):
        copies[i].wait()
    tp_wait(mx, mgat, ssc, rsc, True)
    for i in range(TP):
        r = 32 * (i % 2) + 2 * (i // 2)
        lhs_f[r : r + 2, :] = mgat[i].astype(F32)

    psend[...] = dot(lhs_f[...].astype(BF16), wo_v[...]).astype(BF16)
    for dy, dx in PLANE:
        p = kv_peer(dy, dx)
        to(psend, pr.at[k], ssd.at[p], rsd.at[k], p, t).start()
    pr[k] = psend[...]
    tp_wait(mx, mgat, ssc, rsc, False)
    plane_wait(lambda p: psend, lambda p: pr.at[p], ssd, rsd, True)
    middle = xs[...] + jnp.sum(pr[...].astype(F32), axis=0)
    xs[...] = middle
    scaled = (middle * cg_v[...][None, :]).astype(BF16)
    lhs2[0] = scaled[0:32]
    lhs2[1] = scaled[32:64]
    for i in range(KV):
        mid3[i, 0:2, :] = middle[2 * i : 2 * i + 2]
        mid3[i, 2:4, :] = middle[32 + 2 * i : 34 + 2 * i]

    def product2(i):
        left = lhs2[i]
        rows = xs[pl.ds(pl.multiple_of(i * 32, 32), 32), :]
        pad = jnp.zeros((32, FP - FU), F32)
        return jnp.concatenate(
            [dot(left, w2g[...]), pad, dot(left, w2u[...]), pad, rows * rows], axis=1
        )

    total, scale = reduce_rows(product2, sib_s2, sib_r2, 1, msg2, rb2, ssf, rsf, False)
    gate_part, up_part = scale * total[:, 0:FU], scale * total[:, FP : FP + FU]
    act[...] = (gate_part / (1.0 + jnp.exp(-gate_part)) * up_part).astype(BF16)
    tp_gather(act, agat, ssg, rsg)
    plane_wait(lambda p: psend, lambda p: pr.at[p], ssd, rsd, False)
    sends_done(msg2, rb2, ssf, rsf)
    tp_wait(act, agat, ssg, rsg, True)
    for i in range(TP):
        lhs_d[2 * i : 2 * i + 2, :] = agat[i].astype(F32)

    part = dot(lhs_d[...].astype(BF16), wd_v[...])
    for i in range(KV):
        hmsg[i] = part[4 * i : 4 * i + 4, :].astype(BF16)
    for dy, dx in PLANE:
        p = kv_peer(dy, dx)
        to(hmsg.at[p], hr.at[k], ssh.at[p], rsh.at[k], p, t).start()
    hr[k] = hmsg[k]
    tp_wait(act, agat, ssg, rsg, False)
    plane_wait(lambda p: hmsg.at[p], lambda p: hr.at[p], ssh, rsh, True)
    out[...] = (mid3[k] + jnp.sum(hr[...].astype(F32), axis=0)).astype(BF16)
    plane_wait(lambda p: hmsg.at[p], lambda p: hr.at[p], ssh, rsh, False)


def scratch():
    v = pltpu.VMEM
    dma = pltpu.SemaphoreType.DMA
    return [
        v((4, 128), BF16), v((128,), F32), v((128, 1536), BF16), v((2, 1, 256, 512), F32),
        v((2, 1, 128, 256), BF16), v((2, 1, 128, 512), BF16), v((512,), F32), v((512, 128), BF16),
        v((128,), F32), v((128, FU), BF16), v((128, FU), BF16), v((FU, 128), BF16),
        v((1, 128), F32), pltpu.SMEM((2,), jnp.int32), pltpu.SMEM((1,), F32),
        v((2, 256, 512), BF16), v((2, 256, 512), BF16),
        v((2, 128), F32), v((2, 128), F32), v((2, 128), F32), v((2, 128), F32),
        v((KV, 4, 128), BF16), v((64, 128), F32), v((2, 32, 128), BF16),
        v((32, MSG), BF16), v((32, MSG), BF16), v((ZS, 2, MSG), BF16), v((ZS, 2, MSG), BF16),
        v((2, DV), BF16), v((TP, 2, DV), BF16), v((64, DV), F32),
        v((64, 128), BF16), v((KV, 64, 128), BF16), v((KV, 4, 128), F32), v((2, 32, 128), BF16),
        v((32, MSG), BF16), v((32, MSG), BF16), v((ZS, 2, MSG), BF16), v((ZS, 2, MSG), BF16),
        v((2, FU), BF16), v((TP, 2, FU), BF16), v((64, FU), F32),
        v((KV, 4, 128), BF16), v((KV, 4, 128), BF16),
        dma((18,)), dma((KV,)), dma((KV,)), dma((2,)), dma((2,)), dma((ZS,)), dma((ZS,)),
        dma((TP,)), dma((TP,)), dma((KV,)), dma((KV,)), dma((ZS,)), dma((ZS,)),
        dma((TP,)), dma((TP,)), dma((KV,)), dma((KV,)),
        pltpu.SemaphoreType.REGULAR,
    ]


def local(*args):
    freq = jnp.asarray(
        (10000.0 ** (-np.arange(128, dtype=np.float64) / 128)).astype(np.float32)[None, :]
    )
    return pl.pallas_call(
        kernel,
        out_shape=jax.ShapeDtypeStruct((4, 128), BF16),
        in_specs=[pl.BlockSpec(memory_space=pl.ANY)] * 18,
        out_specs=pl.BlockSpec(memory_space=pltpu.VMEM),
        scratch_shapes=scratch(),
        compiler_params=pltpu.CompilerParams(
            collective_id=0, has_side_effects=True, vmem_limit_bytes=48 * 1024 * 1024
        ),
    )(*args, freq)


def solution(mesh):
    in_specs = (
        P("kv", "tp"), P("tp"), P("tp", "kv"), P("tp", "kv"), P("tp", "kv"), P("tp", "kv"),
        P("kv"), P("tp", "kv", None, None), P("tp", "kv", None, None), P("tp", "kv", None, None),
        P("tp"), P("kv"), P("kv", "tp"), P("tp"), P("tp", "kv"), P("tp", "kv"), P("kv", "tp"),
    )
    return jax.shard_map(
        local, mesh=mesh, in_specs=in_specs, out_specs=P("kv", "tp"), check_vma=False
    )
```

```python
import functools

import jax
import jax.numpy as jnp
import numpy as np
from jax import lax
from jax.experimental import pallas as pl
from jax.experimental.pallas import tpu as pltpu
from jax.sharding import PartitionSpec as P

D = 4096
EPS = 1e-06
KV = 16
ZS = 16
TP = 32
DK = 256
DV = 512
FU = 704
FP = 768
MSG = 1664
UPTO = 99
F32 = jnp.float32
BF16 = jnp.bfloat16
MESH = pl.DeviceIdType.MESH

PLANE = sorted(
    [(dy, dx) for dy in range(4) for dx in range(4) if (dy, dx) != (0, 0)],
    key=lambda o: -(min(o[0], 4 - o[0]) + min(o[1], 4 - o[1])),
)


def dot(a, b):
    return jnp.dot(a, b, preferred_element_type=F32)


def dot_t(a, b):
    return lax.dot_general(a, b, (((1,), (1,)), ((), ())), preferred_element_type=F32)


def sin_cos(a):
    n = jnp.floor(a * np.float32(2.0 / np.pi) + 0.5)
    r = a - n * np.float32(1.5703125)
    r = r - n * np.float32(4.837512969970703125e-4)
    r = r - n * np.float32(7.549789954891882e-8)
    z = r * r
    s = r + r * z * (-1.6666654611e-1 + z * (8.3321608736e-3 - z * 1.9515295891e-4))
    c = 1.0 - 0.5 * z + z * z * (
        4.166664568298827e-2 + z * (-1.388731625493765e-3 + z * 2.443315711809948e-5)
    )
    m = n - 4.0 * jnp.floor(n * 0.25)
    odd = (m == 1.0) | (m == 3.0)
    sine = jnp.where(odd, c, s)
    cosine = jnp.where(odd, s, c)
    sine = jnp.where(m >= 2.0, -sine, sine)
    cosine = jnp.where((m == 1.0) | (m == 2.0), -cosine, cosine)
    return sine, cosine


def kernel(
    hid, mgain, wq, wk, wv, wg, decay, state, kblk, vblk, lens, ggain, wo, cgain, hg, hu, hd, freq,
    out,
    hid_v, mg_v, w1, state_v, kb_v, vb_v, gg_v, wo_v, cg_v, w2g, w2u, wd_v, fr_v, len_s, dec_s,
    sh, sl, sin_v, cos_v, wt_v, carry_v,
    xg, xs, lhs1, sib_s, sib_r, msg, rb, mx, mgat, lhs_f, psend, pr, mid3, lhs2, sib_s2, sib_r2,
    msg2, rb2, act, agat, lhs_d, hmsg, hr,
    lsem, ssa, rsa, sspair, rspair, ssb, rsb, ssc, rsc, ssd, rsd, ssf, rsf, ssg, rsg, ssh, rsh,
    far,
):
    k = lax.axis_index("kv")
    t = lax.axis_index("tp")
    z, c = t // 2, t % 2
    y, x = k // 4, k % 4
    sib = 2 * z + 1 - c
    pending = []

    def kv_peer(dy, dx):
        return ((y + dy) % 4) * 4 + (x + dx) % 4

    def z_peer(i):
        off = 8 - (i + 1) // 2
        sign = (i % 2) * 2 - 1
        return (z + sign * off + 16) % 16

    def drain(n=None):
        for _ in range(len(pending) if n is None else n):
            pending.pop(0)()

    def to(src, dst, ss, rs, kv, tp):
        return pltpu.make_async_remote_copy(
            src_ref=src, dst_ref=dst, send_sem=ss, recv_sem=rs,
            device_id={"kv": kv, "tp": tp}, device_id_type=MESH,
        )

    def signal(sem, kv, tp):
        pl.semaphore_signal(sem, inc=1, device_id={"kv": kv, "tp": tp}, device_id_type=MESH)

    loads = [
        (hid, hid_v), (lens, len_s), (decay, dec_s), (freq, fr_v), (mgain, mg_v),
        (wq, w1.at[:, pl.ds(0, 256)]), (wk, w1.at[:, pl.ds(256, 256)]),
        (wv, w1.at[:, pl.ds(512, 512)]), (wg, w1.at[:, pl.ds(1024, 512)]),
        (state, state_v), (kblk, kb_v), (vblk, vb_v), (ggain, gg_v), (wo, wo_v), (cgain, cg_v),
        (hg, w2g), (hu, w2u), (hd, wd_v),
    ]
    copies = [pltpu.make_async_copy(a, b, lsem.at[i]) for i, (a, b) in enumerate(loads)]
    loaded = [0] * len(loads)

    def need(*ids):
        for i in ids:
            if not loaded[i]:
                copies[i].wait()
                loaded[i] = 1

    barrier = pltpu.get_barrier_semaphore()
    for dy, dx in PLANE:
        signal(barrier, kv_peer(dy, dx), t)
    copies[0].start()

    @pl.loop(0, 16)
    def _(i):
        dz = 4 - (i % 8) // 2
        dz = dz - 2 * dz * (i % 2)
        signal(barrier, k, ((z + dz + 16) % 16) * 2 + i // 8)

    signal(barrier, k, sib)
    for cp in copies[1:]:
        cp.start()

    need(1, 2, 3)
    row = lax.broadcasted_iota(jnp.int32, (2, 128), 0)
    slot = lax.broadcasted_iota(jnp.int32, (2, 128), 1)
    length = jnp.where(row == 0, len_s[0], len_s[1])
    sine, cosine = sin_cos(length.astype(F32) * fr_v[...])
    sin_v[...] = sine
    cos_v[...] = cosine
    filled = length & 127
    rate = dec_s[0]
    wt_v[...] = jnp.where(
        slot < filled, jnp.exp(-rate * (filled - slot).astype(F32)), jnp.zeros((2, 128), F32)
    )
    carry_v[...] = jnp.exp(-rate * (filled + 1).astype(F32))

    need(0)
    pl.semaphore_wait(barrier, 32)

    def stop(value):
        drain()
        need(*range(len(loads)))
        out[...] = jnp.broadcast_to(value, (4, 128)).astype(BF16)

    for sg in (4, 12):
        signal(far, k, ((z + sg) % 16) * 2 + c)
    if UPTO == 0:
        pl.semaphore_wait(far, 2)
        return stop(sin_v[0:1, :])

    def plane_start(src, dst, ss, rs):
        for dy, dx in PLANE:
            p = kv_peer(dy, dx)
            to(src(p), dst.at[k], ss, rs, p, t).start()
        pending.append(lambda: all_done(dst, KV - 1, ss))

    def all_done(buf, n, sem):
        part = buf.at[pl.ds(0, n)]
        pltpu.make_async_copy(part, part, sem).wait()

    plane_start(lambda p: hid_v, xg, ssa, rsa)
    xg[k] = hid_v[...]

    need(9)
    for s in range(2):
        whole = state_v[s, 0]
        high = whole.astype(BF16)
        sh[s] = high
        sl[s] = (whole - high.astype(F32)).astype(BF16)
    need(4, 5, 6, 7, 8)

    all_done(xg, KV - 1, rsa)
    for i in range(KV):
        rows = xg[i].astype(F32)
        xs[2 * i : 2 * i + 2, :] = rows[0:2]
        xs[32 + 2 * i : 34 + 2 * i, :] = rows[2:4]
    if UPTO == 1:
        pl.semaphore_wait(far, 2)
        return stop(xs[0:4, :])

    stream = xs[...]
    scaled = (stream * mg_v[...][None, :]).astype(BF16)
    lhs1[0] = scaled[0:32]
    lhs1[1] = scaled[32:64]

    def pair_sum(product, send, recv, which, msgs):
        def lay_out(rows, dst):
            for i in range(ZS):
                dst[i] = rows[2 * i : 2 * i + 2, :].astype(BF16)

        lay_out(product(1 - c), send)
        pair = to(send, recv, sspair.at[which], rspair.at[which], k, sib)
        pair.start()
        lay_out(product(c), msgs)
        pair.wait()
        msgs[...] = msgs[...] + recv[...]

    def z_scatter(msgs, rbuf, ss, rs):
        @pl.loop(0, 15)
        def _(i):
            p = z_peer(i)
            to(msgs.at[p], rbuf.at[z], ss, rs, k, 2 * p + c).start()

        rbuf[z] = msgs[z]
        pending.append(lambda: all_done(rbuf, ZS - 1, ss))
        all_done(rbuf, ZS - 1, rs)

    def z_total(rbuf):
        total = rbuf[0].astype(F32)
        for i in range(1, ZS):
            total = total + rbuf[i].astype(F32)
        scale = lax.rsqrt(
            jnp.sum(total[:, 1536:1664], axis=1, keepdims=True) * np.float32(1.0 / D) + EPS
        )
        return total, scale

    def product1(i):
        left = lhs1[i]
        rows = xs[pl.ds(pl.multiple_of(i * 32, 32), 32), :]
        return jnp.concatenate([dot(left, w1[...]), rows * rows], axis=1)

    pair_sum(product1, sib_s, sib_r, 0, msg)
    pl.semaphore_wait(far, 2)
    if UPTO == 2:
        return stop(msg[0, :, 0:128].astype(F32)[0:1, :])
    z_scatter(msg, rb, ssb, rsb)
    if UPTO == 3:
        return stop(rb[0, :, 0:128].astype(F32)[0:1, :])
    total, scale = z_total(rb)

    def rounded(v):
        return (scale * v).astype(BF16).astype(F32)

    queries, keys_new = rounded(total[:, 0:256]), rounded(total[:, 256:512])
    values_new, gates = rounded(total[:, 512:1024]), rounded(total[:, 1024:1536])
    sine, cosine = sin_v[...], cos_v[...]

    def rotate(v):
        a, b = v[:, 0:128], v[:, 128:256]
        return jnp.concatenate([a * cosine - b * sine, a * sine + b * cosine], axis=1)

    rot = rotate(queries).astype(BF16)
    rot_w = rot.astype(F32)
    fresh = rotate(keys_new) * np.float32(DK**-0.5)
    need(10, 11, 12)

    def pick(a, b):
        first = lax.broadcasted_iota(jnp.int32, a.shape, 0) == 0
        return jnp.where(first, a, b)

    scores = pick(*[dot_t(rot, kb_v[s, 0]) for s in range(2)])
    bw = (scores * wt_v[...]).astype(BF16)
    block_term = pick(*[dot(bw, vb_v[s, 0]) for s in range(2)])
    state_term = pick(*[dot(rot, sh[s]) + dot(rot, sl[s]) for s in range(2)])
    own_term = jnp.sum(rot_w * fresh, axis=1, keepdims=True) * values_new
    retained = own_term + block_term + carry_v[:, 0:1] * state_term
    centre = jnp.mean(retained, axis=1, keepdims=True)
    off = retained - centre
    spread = jnp.mean(off * off, axis=1, keepdims=True)
    normed = off * lax.rsqrt(spread + EPS)
    silu = gates / (1.0 + jnp.exp(-gates))
    mx[...] = (silu * normed * gg_v[...][None, :]).astype(BF16)
    if UPTO == 4:
        return stop(mx[:, 0:128].astype(F32)[0:1, :])

    def tp_start(src, buf, ss, rs):
        @pl.loop(0, 15)
        def _(i):
            p = z_peer(i)
            for core in range(2):
                to(src, buf.at[t], ss, rs, k, 2 * p + core).start()

        to(src, buf.at[t], ss, rs, k, sib).start()
        buf[t] = src[...]
        pending.append(lambda: all_done(buf, TP - 1, ss))

    tp_start(mx, mgat, ssc, rsc)
    drain(2)
    need(13, 14, 15, 16, 17)
    all_done(mgat, TP - 1, rsc)
    if UPTO == 5:
        return stop(mgat[0, :, 0:128].astype(F32)[0:1, :])
    for i in range(TP):
        r = 32 * (i % 2) + 2 * (i // 2)
        lhs_f[r : r + 2, :] = mgat[i].astype(F32)

    psend[...] = dot(lhs_f[...].astype(BF16), wo_v[...]).astype(BF16)
    if UPTO == 6:
        return stop(psend[0:16, :].astype(F32)[0:1, :])
    plane_start(lambda p: psend, pr, ssd, rsd)
    pr[k] = psend[...]
    drain(1)
    all_done(pr, KV - 1, rsd)
    if UPTO == 7:
        return stop(pr[0, 0:16, :].astype(F32)[0:1, :])
    middle = xs[...] + jnp.sum(pr[...].astype(F32), axis=0)
    xs[...] = middle
    scaled = (middle * cg_v[...][None, :]).astype(BF16)
    lhs2[0] = scaled[0:32]
    lhs2[1] = scaled[32:64]
    for i in range(KV):
        mid3[i, 0:2, :] = middle[2 * i : 2 * i + 2]
        mid3[i, 2:4, :] = middle[32 + 2 * i : 34 + 2 * i]

    def product2(i):
        left = lhs2[i]
        rows = xs[pl.ds(pl.multiple_of(i * 32, 32), 32), :]
        pad = jnp.zeros((32, FP - FU), F32)
        return jnp.concatenate(
            [dot_t(left, w2g[...]), pad, dot_t(left, w2u[...]), pad, rows * rows], axis=1
        )

    pair_sum(product2, sib_s2, sib_r2, 1, msg2)
    if UPTO == 8:
        return stop(msg2[0, :, 0:128].astype(F32)[0:1, :])
    z_scatter(msg2, rb2, ssf, rsf)
    total, scale = z_total(rb2)
    gate_part, up_part = scale * total[:, 0:FU], scale * total[:, FP : FP + FU]
    act[...] = (gate_part / (1.0 + jnp.exp(-gate_part)) * up_part).astype(BF16)
    if UPTO == 9:
        return stop(act[:, 0:128].astype(F32)[0:1, :])
    tp_start(act, agat, ssg, rsg)
    drain(2)
    all_done(agat, TP - 1, rsg)
    if UPTO == 10:
        return stop(agat[0, :, 0:128].astype(F32)[0:1, :])
    for i in range(TP):
        lhs_d[2 * i : 2 * i + 2, :] = agat[i].astype(F32)

    part = dot(lhs_d[...].astype(BF16), wd_v[...])
    for i in range(KV):
        hmsg[i] = part[4 * i : 4 * i + 4, :].astype(BF16)
    if UPTO == 11:
        return stop(hmsg[0].astype(F32))
    plane_start(lambda p: hmsg.at[p], hr, ssh, rsh)
    hr[k] = hmsg[k]
    drain(1)
    all_done(hr, KV - 1, rsh)
    out[...] = (mid3[k] + jnp.sum(hr[...].astype(F32), axis=0)).astype(BF16)
    drain()


def scratch():
    v = pltpu.VMEM
    dma = pltpu.SemaphoreType.DMA
    return [
        v((4, 128), BF16), v((128,), F32), v((128, 1536), BF16), v((2, 1, 256, 512), F32),
        v((2, 1, 128, 256), BF16), v((2, 1, 128, 512), BF16), v((512,), F32), v((512, 128), BF16),
        v((128,), F32), v((FU, 128), BF16), v((FU, 128), BF16), v((FU, 128), BF16),
        v((1, 128), F32), pltpu.SMEM((2,), jnp.int32), pltpu.SMEM((1,), F32),
        v((2, 256, 512), BF16), v((2, 256, 512), BF16),
        v((2, 128), F32), v((2, 128), F32), v((2, 128), F32), v((2, 128), F32),
        v((KV, 4, 128), BF16), v((64, 128), F32), v((2, 32, 128), BF16),
        v((ZS, 2, MSG), BF16), v((ZS, 2, MSG), BF16), v((ZS, 2, MSG), BF16), v((ZS, 2, MSG), BF16),
        v((2, DV), BF16), v((TP, 2, DV), BF16), v((64, DV), F32),
        v((64, 128), BF16), v((KV, 64, 128), BF16), v((KV, 4, 128), F32), v((2, 32, 128), BF16),
        v((ZS, 2, MSG), BF16), v((ZS, 2, MSG), BF16), v((ZS, 2, MSG), BF16), v((ZS, 2, MSG), BF16),
        v((2, FU), BF16), v((TP, 2, FU), BF16), v((64, FU), F32),
        v((KV, 4, 128), BF16), v((KV, 4, 128), BF16),
        dma((18,)), dma, dma, dma((2,)), dma((2,)), *[dma] * 12,
        pltpu.SemaphoreType.REGULAR,
    ]


def local(*args):
    freq = jnp.asarray(
        (10000.0 ** (-np.arange(128, dtype=np.float64) / 128)).astype(np.float32)[None, :]
    )
    args = (*args[:14], args[14].T, args[15].T, args[16])
    return pl.pallas_call(
        kernel,
        out_shape=jax.ShapeDtypeStruct((4, 128), BF16),
        in_specs=[pl.BlockSpec(memory_space=pltpu.HBM)] * 18,
        out_specs=pl.BlockSpec(memory_space=pltpu.VMEM),
        scratch_shapes=scratch(),
        compiler_params=pltpu.CompilerParams(
            collective_id=0, has_side_effects=True, vmem_limit_bytes=58000000
        ),
    )(*args, freq)


def solution(mesh):
    in_specs = (
        P("kv", "tp"), P("tp"), P("tp", "kv"), P("tp", "kv"), P("tp", "kv"), P("tp", "kv"),
        P("kv"), P("tp", "kv", None, None), P("tp", "kv", None, None), P("tp", "kv", None, None),
        P("tp"), P("kv"), P("kv", "tp"), P("tp"), P("tp", "kv"), P("tp", "kv"), P("kv", "tp"),
    )
    return jax.shard_map(
        local, mesh=mesh, in_specs=in_specs, out_specs=P("kv", "tp"), check_vma=False
    )
```

```python
import functools

import jax
import jax.numpy as jnp
import numpy as np
from jax import lax
from jax.experimental import pallas as pl
from jax.experimental.pallas import tpu as pltpu
from jax.sharding import PartitionSpec as P

D = 4096
EPS = 1e-06
KV = 16
ZS = 16
DK = 256
DV = 512
FU = 704
FP = 768
MSG = 1664
UPTO = 99
LIMIT = 56500000
F32 = jnp.float32
BF16 = jnp.bfloat16
MESH = pl.DeviceIdType.MESH

PLANE = sorted(
    [(dy, dx) for dy in range(4) for dx in range(4) if (dy, dx) != (0, 0)],
    key=lambda o: -(min(o[0], 4 - o[0]) + min(o[1], 4 - o[1])),
)


def dot(a, b):
    return jnp.dot(a, b, preferred_element_type=F32)


def dot_t(a, b):
    return lax.dot_general(a, b, (((1,), (1,)), ((), ())), preferred_element_type=F32)


def sin_cos(a):
    n = jnp.floor(a * np.float32(2.0 / np.pi) + 0.5)
    r = a - n * np.float32(1.5703125)
    r = r - n * np.float32(4.837512969970703125e-4)
    r = r - n * np.float32(7.549789954891882e-8)
    z = r * r
    s = r + r * z * (-1.6666654611e-1 + z * (8.3321608736e-3 - z * 1.9515295891e-4))
    c = 1.0 - 0.5 * z + z * z * (
        4.166664568298827e-2 + z * (-1.388731625493765e-3 + z * 2.443315711809948e-5)
    )
    m = n - 4.0 * jnp.floor(n * 0.25)
    odd = (m == 1.0) | (m == 3.0)
    sine = jnp.where(odd, c, s)
    cosine = jnp.where(odd, s, c)
    sine = jnp.where(m >= 2.0, -sine, sine)
    cosine = jnp.where((m == 1.0) | (m == 2.0), -cosine, cosine)
    return sine, cosine


def kernel(
    hid, mgain, wq, wk, wv, wg, decay, state, kblk, vblk, lens, ggain, wo, cgain, hg, hu, hd, freq,
    out,
    hid_v, mg_v, w1, state_v, kb_v, vb_v, gg_v, wo_v, cg_v, w2g, w2u, wd_v, fr_v, len_s, dec_s,
    sh, sl, sin_v, cos_v, wt_v, carry_v,
    xo, xg, xs, msg, rb, mx, mgat, lhs_f, psend, pr, mid3, give, mres, msg2, rb2, act, agat, lhs_d,
    hmsg, hr,
    lsem, wss, wrs, ssa, rsa, ssb, rsb, ssc, rsc, ssd, rsd, ssm, rsm, ssf, rsf, ssg, rsg, ssh, rsh,
    far,
):
    k = lax.axis_index("kv")
    t = lax.axis_index("tp")
    z, c = t // 2, t % 2
    y, x = k // 4, k % 4
    sib = 2 * z + 1 - c
    mine = pl.ds(pl.multiple_of(c * 128, 128), 128)
    pending = []

    def kv_peer(dy, dx):
        return ((y + dy) % 4) * 4 + (x + dx) % 4

    def z_peer(i):
        off = 8 - (i + 1) // 2
        sign = (i % 2) * 2 - 1
        return (z + sign * off + 16) % 16

    def drain(n=None):
        for _ in range(len(pending) if n is None else n):
            pending.pop(0)()

    def to(src, dst, ss, rs, kv, tp):
        return pltpu.make_async_remote_copy(
            src_ref=src, dst_ref=dst, send_sem=ss, recv_sem=rs,
            device_id={"kv": kv, "tp": tp}, device_id_type=MESH,
        )

    def all_done(buf, n, sem):
        part = buf.at[pl.ds(0, n)]
        pltpu.make_async_copy(part, part, sem).wait()

    def signal(sem, kv, tp):
        pl.semaphore_signal(sem, inc=1, device_id={"kv": kv, "tp": tp}, device_id_type=MESH)

    barrier = pltpu.get_barrier_semaphore()
    for dy, dx in PLANE:
        for core in range(2):
            signal(barrier, kv_peer(dy, dx), 2 * z + core)
    for dz in (4, -4, 3, -3, 2, -2, 1, -1):
        signal(barrier, k, ((z + dz + 16) % 16) * 2 + c)
    signal(barrier, k, sib)

    loads = [
        (hid, hid_v), (lens, len_s), (decay, dec_s), (freq, fr_v), (mgain, mg_v.at[c]),
        (wq, w1.at[mine, pl.ds(0, 256)]), (wk, w1.at[mine, pl.ds(256, 256)]),
        (wv, w1.at[mine, pl.ds(512, 512)]), (wg, w1.at[mine, pl.ds(1024, 512)]),
        (state, state_v), (kblk, kb_v), (vblk, vb_v), (ggain, gg_v), (wo, wo_v.at[:, mine]),
        (cgain, cg_v.at[c]), (hg, w2g.at[:, mine]), (hu, w2u.at[:, mine]), (hd, wd_v.at[:, mine]),
    ]
    copies = [pltpu.make_async_copy(a, b, lsem.at[i]) for i, (a, b) in enumerate(loads)]
    loaded = [0] * len(loads)

    def need(*ids):
        for i in ids:
            if not loaded[i]:
                copies[i].wait()
                loaded[i] = 1

    for cp in copies:
        cp.start()
    shared = [
        (mg_v.at[c], 4), (w1.at[mine, :], (5, 6, 7, 8)), (wo_v.at[:, mine], 13), (cg_v.at[c], 14),
        (w2g.at[:, mine], 15), (w2u.at[:, mine], 16), (wd_v.at[:, mine], 17),
    ]
    share = [to(r, r, wss.at[i], wrs.at[i], k, sib) for i, (r, _) in enumerate(shared)]

    need(1, 2, 3)
    row = lax.broadcasted_iota(jnp.int32, (2, 128), 0)
    slot = lax.broadcasted_iota(jnp.int32, (2, 128), 1)
    length = jnp.where(row == 0, len_s[0], len_s[1])
    sine, cosine = sin_cos(length.astype(F32) * fr_v[...])
    sin_v[...] = sine
    cos_v[...] = cosine
    filled = length & 127
    rate = dec_s[0]
    wt_v[...] = jnp.where(
        slot < filled, jnp.exp(-rate * (filled - slot).astype(F32)), jnp.zeros((2, 128), F32)
    )
    carry_v[...] = jnp.exp(-rate * (filled + 1).astype(F32))

    need(0)
    xo[0] = hid_v[0:2, :]
    xo[1] = hid_v[2:4, :]
    pl.semaphore_wait(barrier, 39)

    def stop(value):
        drain()
        need(*range(len(loads)))
        out[...] = jnp.broadcast_to(value, (4, 128)).astype(BF16)

    def both_cores(src, dst, ss, rs):
        for dy, dx in PLANE:
            p = kv_peer(dy, dx)
            for core in range(2):
                to(src(core, p), dst.at[16 * c + k], ss, rs, p, 2 * z + core).start()
        to(src(1 - c, k), dst.at[16 * c + k], ss, rs, k, sib).start()
        pending.append(lambda: all_done(dst, 2 * KV - 1, ss))

    both_cores(lambda core, p: xo.at[core], xg, ssa, rsa)
    for sg in (4, 12):
        signal(far, k, ((z + sg) % 16) * 2 + c)
    xg[16 * c + k] = xo[c]
    for (_, ids), cp in zip(shared, share):
        need(*((ids,) if isinstance(ids, int) else ids))
        cp.start()
    pending.append(lambda: [cp.wait_send() for cp in share])

    need(9)
    for s in range(2):
        whole = state_v[s, 0]
        high = whole.astype(BF16)
        sh[s] = high
        sl[s] = (whole - high.astype(F32)).astype(BF16)
    share[0].wait_recv()
    share[1].wait_recv()

    all_done(xg, 2 * KV - 1, rsa)
    if UPTO == 1:
        pl.semaphore_wait(far, 2)
        [cp.wait_recv() for cp in share[2:]]
        return stop(xs[0:1, 0:128])
    for i in range(KV):
        xs[2 * i : 2 * i + 2, 0:128] = xg[i].astype(F32)
        xs[2 * i : 2 * i + 2, 128:256] = xg[16 + i].astype(F32)

    def both_gains(ref):
        return jnp.concatenate([ref[0], ref[1]], axis=1)

    def squares(v):
        v = v * v
        return v[:, 0:128] + v[:, 128:256]

    def lay_out(rows, dst):
        for i in range(ZS):
            dst[i] = rows[2 * i : 2 * i + 2, :].astype(BF16)

    def z_scatter(msgs, rbuf, ss, rs):
        @pl.loop(0, 15)
        def _(i):
            p = z_peer(i)
            to(msgs.at[p], rbuf.at[z], ss, rs, k, 2 * p + c).start()

        rbuf[z] = msgs[z]
        pending.append(lambda: all_done(rbuf, ZS - 1, ss))
        all_done(rbuf, ZS - 1, rs)

    def z_total(rbuf):
        total = rbuf[0].astype(F32)
        for i in range(1, ZS):
            total = total + rbuf[i].astype(F32)
        scale = lax.rsqrt(
            jnp.sum(total[:, 1536:1664], axis=1, keepdims=True) * np.float32(1.0 / D) + EPS
        )
        return total, scale

    stream = xs[...]
    scaled = (stream * both_gains(mg_v)).astype(BF16)
    lay_out(jnp.concatenate([dot(scaled, w1[...]), squares(stream)], axis=1), msg)
    pl.semaphore_wait(far, 2)
    if UPTO == 2:
        [cp.wait_recv() for cp in share[2:]]
        return stop(msg[0, :, 0:128].astype(F32)[0:1, :])
    z_scatter(msg, rb, ssb, rsb)
    total, scale = z_total(rb)

    def rounded(v):
        return (scale * v).astype(BF16).astype(F32)

    queries, keys_new = rounded(total[:, 0:256]), rounded(total[:, 256:512])
    values_new, gates = rounded(total[:, 512:1024]), rounded(total[:, 1024:1536])
    sine, cosine = sin_v[...], cos_v[...]

    def rotate(v):
        a, b = v[:, 0:128], v[:, 128:256]
        return jnp.concatenate([a * cosine - b * sine, a * sine + b * cosine], axis=1)

    rot = rotate(queries).astype(BF16)
    rot_w = rot.astype(F32)
    fresh = rotate(keys_new) * np.float32(DK**-0.5)
    need(10, 11, 12)

    def pick(a, b):
        first = lax.broadcasted_iota(jnp.int32, a.shape, 0) == 0
        return jnp.where(first, a, b)

    scores = pick(*[dot_t(rot, kb_v[s, 0]) for s in range(2)])
    bw = (scores * wt_v[...]).astype(BF16)
    block_term = pick(*[dot(bw, vb_v[s, 0]) for s in range(2)])
    state_term = pick(*[dot(rot, sh[s]) + dot(rot, sl[s]) for s in range(2)])
    own_term = jnp.sum(rot_w * fresh, axis=1, keepdims=True) * values_new
    retained = own_term + block_term + carry_v[:, 0:1] * state_term
    centre = jnp.mean(retained, axis=1, keepdims=True)
    off = retained - centre
    spread = jnp.mean(off * off, axis=1, keepdims=True)
    normed = off * lax.rsqrt(spread + EPS)
    silu = gates / (1.0 + jnp.exp(-gates))
    mx[...] = (silu * normed * gg_v[...][None, :]).astype(BF16)

    def z_gather(src, buf, ss, rs):
        @pl.loop(0, 15)
        def _(i):
            to(src, buf.at[z], ss, rs, k, 2 * z_peer(i) + c).start()

        buf[z] = src[...]
        drain()
        pending.append(lambda: all_done(buf, ZS - 1, ss))

    z_gather(mx, mgat, ssc, rsc)
    [cp.wait_recv() for cp in share[2:]]
    all_done(mgat, ZS - 1, rsc)
    if UPTO == 5:
        return stop(mgat[0, :, 0:128].astype(F32)[0:1, :])
    for i in range(ZS):
        lhs_f[2 * i : 2 * i + 2, :] = mgat[i].astype(F32)

    psend[...] = dot(lhs_f[...].astype(BF16), wo_v[...]).astype(BF16)
    for dy, dx in PLANE:
        p = kv_peer(dy, dx)
        to(psend, pr.at[k], ssd, rsd, p, t).start()
    pr[k] = psend[...]
    drain()
    pending.append(lambda: all_done(pr, KV - 1, ssd))
    all_done(pr, KV - 1, rsd)
    if UPTO == 7:
        return stop(pr[0, 0:16, 0:128].astype(F32)[0:1, :])
    middle = xs[...] + jnp.sum(pr[...].astype(F32), axis=0)
    scaled = (middle * both_gains(cg_v)).astype(BF16)
    pad = jnp.zeros((32, FP - FU), F32)
    lay_out(
        jnp.concatenate(
            [dot_t(scaled, w2g[...]), pad, dot_t(scaled, w2u[...]), pad, squares(middle)], axis=1
        ),
        msg2,
    )
    if UPTO == 8:
        return stop(msg2[0, :, 0:128].astype(F32)[0:1, :])

    def residual():
        for i in range(KV):
            mid3[i] = middle[2 * i : 2 * i + 2, :]
        rows = mid3[k]
        give[0] = rows[:, 0:128]
        give[1] = rows[:, 128:256]
        mres[c] = give[c]
        to(give.at[1 - c], mres.at[c], ssm, rsm, k, sib).start()

    @pl.loop(0, 15)
    def _(i):
        p = z_peer(i)
        to(msg2.at[p], rb2.at[z], ssf, rsf, k, 2 * p + c).start()

    rb2[z] = msg2[z]
    residual()
    drain()
    all_done(rb2, ZS - 1, rsf)
    pending.append(lambda: all_done(rb2, ZS - 1, ssf))
    other = to(give.at[1 - c], mres.at[1 - c], ssm, rsm, k, sib)
    pending.append(other.wait)
    total, scale = z_total(rb2)
    gate_part, up_part = scale * total[:, 0:FU], scale * total[:, FP : FP + FU]
    act[...] = (gate_part / (1.0 + jnp.exp(-gate_part)) * up_part).astype(BF16)
    if UPTO == 9:
        return stop(act[:, 0:128].astype(F32)[0:1, :])
    z_gather(act, agat, ssg, rsg)
    all_done(agat, ZS - 1, rsg)
    if UPTO == 10:
        return stop(agat[0, :, 0:128].astype(F32)[0:1, :])
    for i in range(ZS):
        lhs_d[2 * i : 2 * i + 2, :] = agat[i].astype(F32)

    part = dot(lhs_d[...].astype(BF16), wd_v[...])
    for i in range(KV):
        hmsg[i] = part[2 * i : 2 * i + 2, 0:128].astype(BF16)
        hmsg[16 + i] = part[2 * i : 2 * i + 2, 128:256].astype(BF16)
    both_cores(lambda core, p: hmsg.at[16 * core + p], hr, ssh, rsh)
    hr[16 * c + k] = hmsg[16 * c + k]
    drain(1)
    all_done(hr, 2 * KV - 1, rsh)
    for half in range(2):
        total = mres[half]
        for i in range(KV):
            total = total + hr[16 * half + i].astype(F32)
        out[2 * half : 2 * half + 2, :] = total.astype(BF16)
    drain()


def scratch():
    v = pltpu.VMEM
    dma = pltpu.SemaphoreType.DMA
    return [
        v((4, 128), BF16), v((2, 1, 128), F32), v((256, 1536), BF16), v((2, 1, 256, 512), F32),
        v((2, 1, 128, 256), BF16), v((2, 1, 128, 512), BF16), v((512,), F32), v((512, 256), BF16),
        v((2, 1, 128), F32), v((FU, 256), BF16), v((FU, 256), BF16), v((FU, 256), BF16),
        v((1, 128), F32), pltpu.SMEM((2,), jnp.int32), pltpu.SMEM((1,), F32),
        v((2, 256, 512), BF16), v((2, 256, 512), BF16),
        v((2, 128), F32), v((2, 128), F32), v((2, 128), F32), v((2, 128), F32),
        v((2, 2, 128), BF16), v((2 * KV, 2, 128), BF16), v((32, 256), F32),
        v((ZS, 2, MSG), BF16), v((ZS, 2, MSG), BF16), v((2, DV), BF16), v((ZS, 2, DV), BF16),
        v((32, DV), F32), v((32, 256), BF16), v((KV, 32, 256), BF16), v((KV, 2, 256), F32),
        v((2, 2, 128), F32), v((2, 2, 128), F32), v((ZS, 2, MSG), BF16), v((ZS, 2, MSG), BF16),
        v((2, FU), BF16), v((ZS, 2, FU), BF16), v((32, FU), F32),
        v((2 * KV, 2, 128), BF16), v((2 * KV, 2, 128), BF16),
        dma((18,)), dma((7,)), dma((7,)), *[dma] * 16, pltpu.SemaphoreType.REGULAR,
    ]


def local(*args):
    freq = jnp.asarray(
        (10000.0 ** (-np.arange(128, dtype=np.float64) / 128)).astype(np.float32)[None, :]
    )
    args = list(args)
    for i in (1, 13):
        args[i] = args[i].reshape(1, 128)
    for i in (14, 15):
        args[i] = args[i].T
    return pl.pallas_call(
        kernel,
        out_shape=jax.ShapeDtypeStruct((4, 128), BF16),
        in_specs=[pl.BlockSpec(memory_space=pltpu.HBM)] * 18,
        out_specs=pl.BlockSpec(memory_space=pltpu.VMEM),
        scratch_shapes=scratch(),
        compiler_params=pltpu.CompilerParams(
            collective_id=0, has_side_effects=True, vmem_limit_bytes=LIMIT
        ),
    )(*args, freq)


def solution(mesh):
    in_specs = (
        P("kv", "tp"), P("tp"), P("tp", "kv"), P("tp", "kv"), P("tp", "kv"), P("tp", "kv"),
        P("kv"), P("tp", "kv", None, None), P("tp", "kv", None, None), P("tp", "kv", None, None),
        P("tp"), P("kv"), P("kv", "tp"), P("tp"), P("tp", "kv"), P("tp", "kv"), P("kv", "tp"),
    )
    return jax.shard_map(
        local, mesh=mesh, in_specs=in_specs, out_specs=P("kv", "tp"), check_vma=False
    )
```

```python
import functools

import jax
import jax.numpy as jnp
import numpy as np
from jax import lax
from jax.experimental import pallas as pl
from jax.experimental.pallas import tpu as pltpu
from jax.sharding import PartitionSpec as P

D = 4096
EPS = 1e-06
KV = 16
ZS = 16
DK = 256
DV = 512
FU = 704
FP = 768
MSG = 1664
MSG2 = 1536
UPTO = 99
LIMIT = 58000000
F32 = jnp.float32
BF16 = jnp.bfloat16
MESH = pl.DeviceIdType.MESH

PLANE = sorted(
    [(dy, dx) for dy in range(4) for dx in range(4) if (dy, dx) != (0, 0)],
    key=lambda o: -(min(o[0], 4 - o[0]) + min(o[1], 4 - o[1])),
)


def dot(a, b):
    return jnp.dot(a, b, preferred_element_type=F32)


def dot_t(a, b):
    return lax.dot_general(a, b, (((1,), (1,)), ((), ())), preferred_element_type=F32)


def sin_cos(a):
    n = jnp.floor(a * np.float32(2.0 / np.pi) + 0.5)
    r = a - n * np.float32(1.5703125)
    r = r - n * np.float32(4.837512969970703125e-4)
    r = r - n * np.float32(7.549789954891882e-8)
    z = r * r
    s = r + r * z * (-1.6666654611e-1 + z * (8.3321608736e-3 - z * 1.9515295891e-4))
    c = 1.0 - 0.5 * z + z * z * (
        4.166664568298827e-2 + z * (-1.388731625493765e-3 + z * 2.443315711809948e-5)
    )
    m = n - 4.0 * jnp.floor(n * 0.25)
    odd = (m == 1.0) | (m == 3.0)
    sine = jnp.where(odd, c, s)
    cosine = jnp.where(odd, s, c)
    sine = jnp.where(m >= 2.0, -sine, sine)
    cosine = jnp.where((m == 1.0) | (m == 2.0), -cosine, cosine)
    return sine, cosine


def kernel(
    hid, mgain, wq, wk, wv, wg, decay, state, kblk, vblk, lens, ggain, wo, cgain, hg, hu, hd, freq,
    out,
    hid_v, mg_v, w1, state_v, kb_v, vb_v, gg_v, wo_v, cg_v, w2g, w2u, wd_v, fr_v, len_s, dec_s,
    sh, sl, sin_v, cos_v, wt_v, carry_v,
    xo, xg, xs, msg, rb, mx, mgat, lhs_f, psend, pr, mid3, give, mres, msg2, rb2, act, agat, lhs_d,
    hmsg, hr,
    lsem, wss, wrs, ssa, rsa, ssb, rsb, ssc, rsc, ssd, rsd, ssm, rsm, ssf, rsf, ssg, rsg, ssh, rsh,
    far,
):
    k = lax.axis_index("kv")
    t = lax.axis_index("tp")
    z, c = t // 2, t % 2
    y, x = k // 4, k % 4
    sib = 2 * z + 1 - c
    mine = pl.ds(pl.multiple_of(c * 128, 128), 128)
    pending = []

    def kv_peer(dy, dx):
        return ((y + dy) % 4) * 4 + (x + dx) % 4

    def z_peer(i):
        off = 8 - (i + 1) // 2
        sign = (i % 2) * 2 - 1
        return (z + sign * off + 16) % 16

    def drain(n=None):
        for _ in range(len(pending) if n is None else n):
            pending.pop(0)()

    def to(src, dst, ss, rs, kv, tp):
        return pltpu.make_async_remote_copy(
            src_ref=src, dst_ref=dst, send_sem=ss, recv_sem=rs,
            device_id={"kv": kv, "tp": tp}, device_id_type=MESH,
        )

    def all_done(buf, n, sem):
        part = buf.at[pl.ds(0, n)]
        pltpu.make_async_copy(part, part, sem).wait()

    def signal(sem, kv, tp):
        pl.semaphore_signal(sem, inc=1, device_id={"kv": kv, "tp": tp}, device_id_type=MESH)

    barrier = pltpu.get_barrier_semaphore()
    for dy, dx in PLANE:
        for core in range(2):
            signal(barrier, kv_peer(dy, dx), 2 * z + core)
    for dz in (4, -4, 3, -3, 2, -2, 1, -1):
        signal(barrier, k, ((z + dz + 16) % 16) * 2 + c)
    signal(barrier, k, sib)

    loads = [
        (hid, hid_v), (lens, len_s), (decay, dec_s), (freq, fr_v), (mgain, mg_v.at[c]),
        (wq, w1.at[mine, pl.ds(0, 256)]), (wk, w1.at[mine, pl.ds(256, 256)]),
        (wv, w1.at[mine, pl.ds(512, 512)]), (wg, w1.at[mine, pl.ds(1024, 512)]),
        (state, state_v), (kblk, kb_v), (vblk, vb_v), (ggain, gg_v), (wo, wo_v.at[:, mine]),
        (cgain, cg_v.at[c]), (hg, w2g.at[:, mine]), (hu, w2u.at[:, mine]), (hd, wd_v.at[:, mine]),
    ]
    copies = [pltpu.make_async_copy(a, b, lsem.at[i]) for i, (a, b) in enumerate(loads)]
    loaded = [0] * len(loads)

    def need(*ids):
        for i in ids:
            if not loaded[i]:
                copies[i].wait()
                loaded[i] = 1

    for cp in copies:
        cp.start()
    shared = [
        (mg_v.at[c], 4), (w1.at[mine, :], (5, 6, 7, 8)), (wo_v.at[:, mine], 13), (cg_v.at[c], 14),
        (w2g.at[:, mine], 15), (w2u.at[:, mine], 16), (wd_v.at[:, mine], 17),
    ]
    share = [to(r, r, wss.at[i], wrs.at[i], k, sib) for i, (r, _) in enumerate(shared)]

    need(1, 2, 3)
    row = lax.broadcasted_iota(jnp.int32, (2, 128), 0)
    slot = lax.broadcasted_iota(jnp.int32, (2, 128), 1)
    length = jnp.where(row == 0, len_s[0], len_s[1])
    sine, cosine = sin_cos(length.astype(F32) * fr_v[...])
    sin_v[...] = sine
    cos_v[...] = cosine
    filled = length & 127
    rate = dec_s[0]
    wt_v[...] = jnp.where(
        slot < filled, jnp.exp(-rate * (filled - slot).astype(F32)), jnp.zeros((2, 128), F32)
    )
    carry_v[...] = jnp.exp(-rate * (filled + 1).astype(F32))

    need(0)
    xo[0] = hid_v[0:2, :]
    xo[1] = hid_v[2:4, :]
    pl.semaphore_wait(barrier, 39)

    def stop(value):
        drain()
        need(*range(len(loads)))
        out[...] = jnp.broadcast_to(value, (4, 128)).astype(BF16)

    def both_cores(src, dst, ss, rs):
        for dy, dx in PLANE:
            p = kv_peer(dy, dx)
            for core in range(2):
                to(src(core, p), dst.at[16 * c + k], ss, rs, p, 2 * z + core).start()
        to(src(1 - c, k), dst.at[16 * c + k], ss, rs, k, sib).start()
        pending.append(lambda: all_done(dst, 2 * KV - 1, ss))

    both_cores(lambda core, p: xo.at[core], xg, ssa, rsa)
    for sg in (4, 12):
        signal(far, k, ((z + sg) % 16) * 2 + c)
    xg[16 * c + k] = xo[c]
    for (_, ids), cp in zip(shared, share):
        need(*((ids,) if isinstance(ids, int) else ids))
        cp.start()
    pending.append(lambda: [cp.wait_send() for cp in share])

    need(9)
    for s in range(2):
        whole = state_v[s, 0]
        high = whole.astype(BF16)
        sh[s] = high
        sl[s] = (whole - high.astype(F32)).astype(BF16)
    share[0].wait_recv()
    share[1].wait_recv()

    all_done(xg, 2 * KV - 1, rsa)
    if UPTO == 1:
        pl.semaphore_wait(far, 2)
        [cp.wait_recv() for cp in share[2:]]
        return stop(xs[0:1, 0:128])
    for i in range(KV):
        xs[2 * i : 2 * i + 2, 0:128] = xg[i].astype(F32)
        xs[2 * i : 2 * i + 2, 128:256] = xg[16 + i].astype(F32)

    def both_gains(ref):
        return jnp.concatenate([ref[0], ref[1]], axis=1)

    def squares(v):
        v = v * v
        return v[:, 0:128] + v[:, 128:256]

    def lay_out(rows, dst):
        for i in range(ZS):
            dst[i] = rows[2 * i : 2 * i + 2, :].astype(BF16)

    def z_scatter(msgs, rbuf, ss, rs):
        @pl.loop(0, 15)
        def _(i):
            p = z_peer(i)
            to(msgs.at[p], rbuf.at[z], ss, rs, k, 2 * p + c).start()

        rbuf[z] = msgs[z]
        pending.append(lambda: all_done(rbuf, ZS - 1, ss))
        all_done(rbuf, ZS - 1, rs)

    def z_total(rbuf, first, last):
        total = rbuf[0].astype(F32)
        for i in range(1, ZS):
            total = total + rbuf[i].astype(F32)
        scale = lax.rsqrt(
            jnp.sum(total[:, first:last], axis=1, keepdims=True) * np.float32(1.0 / D) + EPS
        )
        return total, scale

    stream = xs[...]
    scaled = (stream * both_gains(mg_v)).astype(BF16)
    lay_out(jnp.concatenate([dot(scaled, w1[...]), squares(stream)], axis=1), msg)
    pl.semaphore_wait(far, 2)
    if UPTO == 2:
        [cp.wait_recv() for cp in share[2:]]
        return stop(msg[0, :, 0:128].astype(F32)[0:1, :])
    z_scatter(msg, rb, ssb, rsb)
    total, scale = z_total(rb, 1536, 1664)

    def rounded(v):
        return (scale * v).astype(BF16).astype(F32)

    queries, keys_new = rounded(total[:, 0:256]), rounded(total[:, 256:512])
    values_new, gates = rounded(total[:, 512:1024]), rounded(total[:, 1024:1536])
    sine, cosine = sin_v[...], cos_v[...]

    def rotate(v):
        a, b = v[:, 0:128], v[:, 128:256]
        return jnp.concatenate([a * cosine - b * sine, a * sine + b * cosine], axis=1)

    rot = rotate(queries).astype(BF16)
    rot_w = rot.astype(F32)
    fresh = rotate(keys_new) * np.float32(DK**-0.5)
    need(10, 11, 12)

    def pick(a, b):
        first = lax.broadcasted_iota(jnp.int32, a.shape, 0) == 0
        return jnp.where(first, a, b)

    scores = pick(*[dot_t(rot, kb_v[s, 0]) for s in range(2)])
    bw = (scores * wt_v[...]).astype(BF16)
    block_term = pick(*[dot(bw, vb_v[s, 0]) for s in range(2)])
    state_term = pick(*[dot(rot, sh[s]) + dot(rot, sl[s]) for s in range(2)])
    own_term = jnp.sum(rot_w * fresh, axis=1, keepdims=True) * values_new
    retained = own_term + block_term + carry_v[:, 0:1] * state_term
    centre = jnp.mean(retained, axis=1, keepdims=True)
    off = retained - centre
    spread = jnp.mean(off * off, axis=1, keepdims=True)
    normed = off * lax.rsqrt(spread + EPS)
    silu = gates / (1.0 + jnp.exp(-gates))
    mx[...] = (silu * normed * gg_v[...][None, :]).astype(BF16)

    def z_gather(src, buf, ss, rs):
        @pl.loop(0, 15)
        def _(i):
            to(src, buf.at[z], ss, rs, k, 2 * z_peer(i) + c).start()

        buf[z] = src[...]
        drain()
        pending.append(lambda: all_done(buf, ZS - 1, ss))

    z_gather(mx, mgat, ssc, rsc)
    [cp.wait_recv() for cp in share[2:]]
    all_done(mgat, ZS - 1, rsc)
    if UPTO == 5:
        return stop(mgat[0, :, 0:128].astype(F32)[0:1, :])
    for i in range(ZS):
        lhs_f[2 * i : 2 * i + 2, :] = mgat[i].astype(F32)

    psend[...] = dot(lhs_f[...].astype(BF16), wo_v[...]).astype(BF16)
    for dy, dx in PLANE:
        p = kv_peer(dy, dx)
        to(psend, pr.at[k], ssd, rsd, p, t).start()
    pr[k] = psend[...]
    drain()
    pending.append(lambda: all_done(pr, KV - 1, ssd))
    all_done(pr, KV - 1, rsd)
    if UPTO == 7:
        return stop(pr[0, 0:16, 0:128].astype(F32)[0:1, :])
    middle = xs[...] + jnp.sum(pr[...].astype(F32), axis=0)
    scaled = (middle * both_gains(cg_v)).astype(BF16)
    pad = jnp.zeros((32, FP - FU), F32)
    folded = squares(middle)
    folded = folded[:, 0:64] + folded[:, 64:128]
    lay_out(
        jnp.concatenate(
            [dot_t(scaled, w2g[...]), folded, dot_t(scaled, w2u[...]), pad], axis=1
        ),
        msg2,
    )
    if UPTO == 8:
        return stop(msg2[0, :, 0:128].astype(F32)[0:1, :])

    def residual():
        for i in range(KV):
            mid3[i] = middle[2 * i : 2 * i + 2, :]
        rows = mid3[k]
        give[0] = rows[:, 0:128]
        give[1] = rows[:, 128:256]
        mres[c] = give[c]
        to(give.at[1 - c], mres.at[c], ssm, rsm, k, sib).start()

    @pl.loop(0, 15)
    def _(i):
        p = z_peer(i)
        to(msg2.at[p], rb2.at[z], ssf, rsf, k, 2 * p + c).start()

    rb2[z] = msg2[z]
    residual()
    drain()
    all_done(rb2, ZS - 1, rsf)
    pending.append(lambda: all_done(rb2, ZS - 1, ssf))
    other = to(give.at[1 - c], mres.at[1 - c], ssm, rsm, k, sib)
    pending.append(other.wait)
    total, scale = z_total(rb2, FU, FP)
    gate_part, up_part = scale * total[:, 0:FU], scale * total[:, FP : FP + FU]
    act[...] = (gate_part / (1.0 + jnp.exp(-gate_part)) * up_part).astype(BF16)
    if UPTO == 9:
        return stop(act[:, 0:128].astype(F32)[0:1, :])
    z_gather(act, agat, ssg, rsg)
    all_done(agat, ZS - 1, rsg)
    if UPTO == 10:
        return stop(agat[0, :, 0:128].astype(F32)[0:1, :])
    for i in range(ZS):
        lhs_d[2 * i : 2 * i + 2, :] = agat[i].astype(F32)

    part = dot(lhs_d[...].astype(BF16), wd_v[...])
    for i in range(KV):
        hmsg[i] = part[2 * i : 2 * i + 2, 0:128].astype(BF16)
        hmsg[16 + i] = part[2 * i : 2 * i + 2, 128:256].astype(BF16)
    both_cores(lambda core, p: hmsg.at[16 * core + p], hr, ssh, rsh)
    hr[16 * c + k] = hmsg[16 * c + k]
    drain(1)
    all_done(hr, 2 * KV - 1, rsh)
    for half in range(2):
        total = mres[half]
        for i in range(KV):
            total = total + hr[16 * half + i].astype(F32)
        out[2 * half : 2 * half + 2, :] = total.astype(BF16)
    drain()


def scratch():
    v = pltpu.VMEM
    dma = pltpu.SemaphoreType.DMA
    return [
        v((4, 128), BF16), v((2, 1, 128), F32), v((256, 1536), BF16), v((2, 1, 256, 512), F32),
        v((2, 1, 128, 256), BF16), v((2, 1, 128, 512), BF16), v((512,), F32), v((512, 256), BF16),
        v((2, 1, 128), F32), v((FU, 256), BF16), v((FU, 256), BF16), v((FU, 256), BF16),
        v((1, 128), F32), pltpu.SMEM((2,), jnp.int32), pltpu.SMEM((1,), F32),
        v((2, 256, 512), BF16), v((2, 256, 512), BF16),
        v((2, 128), F32), v((2, 128), F32), v((2, 128), F32), v((2, 128), F32),
        v((2, 2, 128), BF16), v((2 * KV, 2, 128), BF16), v((32, 256), F32),
        v((ZS, 2, MSG), BF16), v((ZS, 2, MSG), BF16), v((2, DV), BF16), v((ZS, 2, DV), BF16),
        v((32, DV), F32), v((32, 256), BF16), v((KV, 32, 256), BF16), v((KV, 2, 256), F32),
        v((2, 2, 128), F32), v((2, 2, 128), F32), v((ZS, 2, MSG2), BF16), v((ZS, 2, MSG2), BF16),
        v((2, FU), BF16), v((ZS, 2, FU), BF16), v((32, FU), F32),
        v((2 * KV, 2, 128), BF16), v((2 * KV, 2, 128), BF16),
        dma((18,)), dma((7,)), dma((7,)), *[dma] * 16, pltpu.SemaphoreType.REGULAR,
    ]


def local(*args):
    freq = jnp.asarray(
        (10000.0 ** (-np.arange(128, dtype=np.float64) / 128)).astype(np.float32)[None, :]
    )
    args = list(args)
    for i in (1, 13):
        args[i] = args[i].reshape(1, 128)
    for i in (14, 15):
        args[i] = args[i].T
    return pl.pallas_call(
        kernel,
        out_shape=pltpu.VMEM((4, 128), BF16),
        in_specs=[pl.BlockSpec(memory_space=pltpu.HBM)] * 18,
        out_specs=pl.BlockSpec(memory_space=pltpu.VMEM),
        scratch_shapes=scratch(),
        compiler_params=pltpu.CompilerParams(
            collective_id=0, has_side_effects=True, vmem_limit_bytes=LIMIT
        ),
    )(*args, freq)


def solution(mesh):
    in_specs = (
        P("kv", "tp"), P("tp"), P("tp", "kv"), P("tp", "kv"), P("tp", "kv"), P("tp", "kv"),
        P("kv"), P("tp", "kv", None, None), P("tp", "kv", None, None), P("tp", "kv", None, None),
        P("tp"), P("kv"), P("kv", "tp"), P("tp"), P("tp", "kv"), P("tp", "kv"), P("kv", "tp"),
    )
    return jax.shard_map(
        local, mesh=mesh, in_specs=in_specs, out_specs=P("kv", "tp"), check_vma=False
    )
```
